32 devices in a mesh: fs: 4 (over z), rep: 4 (over y, x), tp: 2 (over core).
Axes of the slice: x: 2, y: 2, z: 4, core: 2. Of those that a mesh axis runs over, the one named last changes fastest.
Arguments:
- mixer_out: bfloat16 [16384, 1536], P(('fs', 'rep')), may hold values from -6 to 6
- out_grad: bfloat16 [16384, 4096], P(('fs', 'rep'), 'tp'), may hold values from -0.046875 to 0.046875
- factors: bfloat16 [1536, 256], P(('fs', 'rep')), may hold values from -0.15625 to 0.15625
- weight: float32 [1536, 4096], P(('fs', 'rep'), 'tp'), may hold values from -0.15625 to 0.15625
- first_moment: float32 [256, 4096], P(('fs', 'rep'), 'tp'), may hold values from -6 to 6
- second_moment: float32 [256, 4096], P(('fs', 'rep'), 'tp'), may hold values from 0.05 to 2
Outputs:
- new_weight: float32 [1536, 4096], P(('fs', 'rep'), 'tp')
- update: float32 [1536, 4096], P(('fs', 'rep'), 'tp')
- new_first: float32 [256, 4096], P(('fs', 'rep'), 'tp')
- new_second: float32 [256, 4096], P(('fs', 'rep'), 'tp')
- weight_copy: bfloat16 [1536, 4096], P(None, 'tp')
The draws below stay inside these ranges and needn't reach their ends.
All inputs are finite; a program needn't handle non-finite values.
Results may differ from the reference program's by a relative error of at most 0.0034.
Values may be sent and summed in bfloat16 or wider, within the bound.
A program may use at most 64 MiB of HBM per device.

```python
import math
import jax
import jax.numpy as jnp

D = 4096
DH = 1536
RANK = 256
TOK_DEV = 1024
TOKENS = 16384
N_FS = 4
N_REP = 4


def raised(result, rng, source, target, shards_of, factor):
    owner, partner = [(jnp.arange(result.shape[dim]) // (result.shape[dim] // shards_of)).reshape([-1 if axis == dim else 1 for axis in range(result.ndim)]) for dim in (source, target)]
    chosen = jax.random.permutation(rng, shards_of)[partner]
    strong = (owner == chosen) | (owner == (partner + shards_of // 2) % shards_of)
    return jnp.where(strong, factor * result, result)


def block_levels(own_key, dims, cuts, smallest, high):
    def one(axis_at, blocks):
        draws = jax.random.uniform(jax.random.fold_in(jax.random.fold_in(own_key, 6), axis_at), (blocks,), jnp.float32, smallest / len(cuts), high / len(cuts))
        return jnp.repeat(jnp.exp(draws), dims[axis_at] // blocks).reshape((-1,) + (1,) * (len(dims) - axis_at - 1))

    level = one(*cuts[0])
    for cut in cuts[1:]:
        level = level * one(*cut)
    return level


def noise(own_key, dims, scale, limit, pieces=(), dtype=jnp.bfloat16):
    drawn = jax.random.normal(own_key, dims, jnp.float32) * scale
    if len(pieces) > 0:
        drawn = block_levels(own_key, dims, pieces, -0.22, 0.18) * drawn
    return jnp.clip(drawn, min=-limit, max=limit).astype(dtype)


def bell_draw_with(stream_key, dims, spread, most, pieces, heavy, kind=jnp.bfloat16):
    entries = spread * jax.random.normal(stream_key, dims, jnp.float32)
    if pieces:
        entries = entries * block_levels(stream_key, dims, pieces, -0.22, 0.18)
    return jnp.clip(raised(entries, jax.random.fold_in(stream_key, 3), *heavy), -most, most).astype(kind)


def setup_inputs(seed: int = 0) -> dict:
    arg_keys = jax.random.split(jax.random.key(seed), 7)
    return {
        "mixer_out": bell_draw_with(arg_keys[0], (TOKENS, DH), 1.0, 6.0, ((0, 16),), (0, 1, 16, 2.0)),
        "out_grad": noise(arg_keys[1], (TOKENS, D), ((TOK_DEV * N_FS * N_REP) ** -0.5), 0.046875, ((0, 16), (1, 2))),
        "factors": noise(arg_keys[2], (DH, RANK), DH ** -0.5, 0.15625, ((0, 16),)),
        "weight": noise(arg_keys[3], (DH, D), DH ** -0.5, 0.15625, ((0, 16), (1, 2)), jnp.float32),
        "first_moment": noise(arg_keys[4], (RANK, D), 1.0, 6.0, ((0, 16), (1, 2)), jnp.float32),
        "second_moment": jnp.clip(jnp.exp(math.log(2.0) - 3.6888794 * jax.random.uniform(arg_keys[5], (RANK, D), jnp.float32) ** block_levels(arg_keys[5], (RANK, D), ((0, 16), (1, 2)), -0.2, 0.2)), 0.05, 2.0),
    }


def reference(mixer_out, out_grad, factors, weight, first_moment, second_moment):
    gradient = jnp.dot(mixer_out.T, out_grad, preferred_element_type=jnp.float32)
    grad_low = gradient.astype(jnp.bfloat16)
    projected = jnp.dot(factors.T, grad_low, preferred_element_type=jnp.float32)
    new_first = 0.8 * first_moment + 0.2 * projected
    new_second = 0.9 * second_moment + 0.1 * projected * projected
    direction = new_first / (jnp.sqrt(new_second) + 1e-08)
    dir_low = direction.astype(jnp.bfloat16)
    proj_low = projected.astype(jnp.bfloat16)
    dir_wide = dir_low.astype(jnp.float32)
    proj_wide = proj_low.astype(jnp.float32)
    scale_ratio = jnp.sqrt(jnp.sum(dir_wide * dir_wide)) / jnp.sqrt(jnp.sum(proj_wide * proj_wide) + 1e-06)
    back_dir = jnp.dot(factors, dir_low, preferred_element_type=jnp.float32)
    back_proj = jnp.dot(factors, proj_low, preferred_element_type=jnp.float32)
    update = back_dir + scale_ratio * (gradient - back_proj)
    new_weight = weight - 0.01 * update
    weight_copy = new_weight.astype(jnp.bfloat16)
    return (new_weight, update, new_first, new_second, weight_copy)
```

```python
import functools

import jax
import jax.numpy as jnp
from jax import lax
from jax.experimental import pallas as pl
from jax.experimental.pallas import tpu as pltpu
from jax.sharding import PartitionSpec as P

MESH = pl.DeviceIdType.MESH
LANES = 128
TILE = 256


def contract_rows(left, right):
    return lax.dot_general(
        left, right, (((0,), (0,)), ((), ())), preferred_element_type=jnp.float32
    )


def fused_kernel(
    Z, R, T,
    m_ref, o_ref, f_ref, w_ref, m1_ref, m2_ref,
    nw_ref, upd_ref, nf_ref, ns_ref, wc_ref,
    mt, send1, recv1, own, send2, recv2, grad, f_all, m1_all, m2_all,
    nf_col, ns_col, upd_col, stat, stat_all,
    s1_send, s1_recv, s2_send, s2_recv,
    fa_send, fa_recv, ma_send, ma_recv, mb_send, mb_recv,
    st_send, st_recv, nf_send, nf_recv, ns_send, ns_recv, up_send, up_recv,
    gz_send, gz_recv, gr_send, gr_recv,
):
    N = Z * R
    z, r, t = lax.axis_index("fs"), lax.axis_index("rep"), lax.axis_index("tp")
    me = z * R + r
    every = me * T + t
    DH = m_ref.shape[1]
    FR = f_ref.shape[0]
    MR = m1_ref.shape[0]

    def device(zz, rr, tt):
        return {"fs": zz, "rep": rr, "tp": tt}

    def peer(p):
        q = lax.rem(me + p, N)
        return q, q // R, lax.rem(q, R)

    def column(zz, rr):
        return pl.ds(pl.multiple_of((rr * Z + zz) * LANES, LANES), LANES)

    def rows(q, size):
        return pl.ds(pl.multiple_of(q * size, size), size)

    barrier = pltpu.get_barrier_semaphore()

    def greet(p, carry):
        q = lax.rem(every + p, N * T)
        d = q // T
        pl.semaphore_signal(
            barrier, inc=1, device_id=device(d // R, lax.rem(d, R), lax.rem(q, T)), device_id_type=MESH
        )
        return carry

    lax.fori_loop(1, N * T, greet, 0)

    def turn(i, carry):
        part = pl.ds(pl.multiple_of(i * TILE, TILE), TILE)
        mt[part, :] = m_ref[:, part].T
        return carry

    lax.fori_loop(0, DH // TILE, turn, 0)
    pl.semaphore_wait(barrier, N * T - 1)

    def product(zz, rr, store):
        cols = column(zz, rr)

        def tile(i, carry):
            part = pl.ds(pl.multiple_of(i * TILE, TILE), TILE)
            store(part, jnp.dot(mt[part, :], o_ref[:, cols], preferred_element_type=jnp.float32))
            return carry

        lax.fori_loop(0, DH // TILE, tile, 0)

    def first(rr, zz, src):
        return pltpu.make_async_remote_copy(
            src_ref=send1.at[rr, zz], dst_ref=recv1.at[src, zz],
            send_sem=s1_send.at[rr, zz], recv_sem=s1_recv.at[src, zz],
            device_id=device(z, rr, t), device_id_type=MESH,
        )

    def second(zz, src):
        return pltpu.make_async_remote_copy(
            src_ref=send2.at[zz], dst_ref=recv2.at[src],
            send_sem=s2_send.at[zz], recv_sem=s2_recv.at[src],
            device_id=device(zz, r, t), device_id_type=MESH,
        )

    def phase1(i, carry):
        zz = lax.rem(z + 1 + i // (R - 1), Z)
        rr = lax.rem(r + 1 + lax.rem(i, R - 1), R)

        def store(part, value):
            send1[rr, zz, part, :] = value.astype(jnp.bfloat16)

        product(zz, rr, store)
        first(rr, zz, r).start()
        return carry

    lax.fori_loop(0, Z * (R - 1), phase1, 0)

    def f_copy(q, zz, rr, slot):
        return pltpu.make_async_remote_copy(
            src_ref=f_ref, dst_ref=f_all.at[rows(slot, FR), :],
            send_sem=fa_send.at[q], recv_sem=fa_recv.at[slot],
            device_id=device(zz, rr, t), device_id_type=MESH,
        )

    def m_copy(src, dst, ss, rs, q, zz, rr, slot):
        return pltpu.make_async_remote_copy(
            src_ref=src.at[:, column(zz, rr)], dst_ref=dst.at[rows(slot, MR), :],
            send_sem=ss.at[q], recv_sem=rs.at[slot],
            device_id=device(zz, rr, t), device_id_type=MESH,
        )

    def spread(p, carry):
        q, zz, rr = peer(p)
        f_copy(q, zz, rr, me).start()
        m_copy(m1_ref, m1_all, ma_send, ma_recv, q, zz, rr, me).start()
        m_copy(m2_ref, m2_all, mb_send, mb_recv, q, zz, rr, me).start()
        return carry

    lax.fori_loop(1, N, spread, 0)
    f_all[rows(me, FR), :] = f_ref[...]
    m1_all[rows(me, MR), :] = m1_ref[:, column(z, r)]
    m2_all[rows(me, MR), :] = m2_ref[:, column(z, r)]

    def own_block(i, carry):
        def store(part, value):
            own[i, part, :] = value

        product(i, r, store)
        return carry

    lax.fori_loop(0, Z, own_block, 0)

    def join(zz, store):
        def wait(d, carry):
            src = lax.rem(r + d, R)
            first(src, zz, src).wait_recv()
            return carry

        lax.fori_loop(1, R, wait, 0)

        def tile(i, carry):
            part = pl.ds(pl.multiple_of(i * TILE, TILE), TILE)
            total = own[zz, part, :]
            for d in range(1, R):
                total = total + recv1[lax.rem(r + d, R), zz, part, :].astype(jnp.float32)
            store(part, total)
            return carry

        lax.fori_loop(0, DH // TILE, tile, 0)

    def phase2(e, carry):
        zz = lax.rem(z + e, Z)

        def store(part, value):
            send2[zz, part, :] = value.astype(jnp.bfloat16)

        join(zz, store)
        second(zz, z).start()
        return carry

    lax.fori_loop(1, Z, phase2, 0)

    def store_own(part, value):
        grad[part, :] = value

    join(z, store_own)

    def wait_spread(p, carry):
        q, zz, rr = peer(p)
        f_copy(q, zz, rr, q).wait()
        m_copy(m1_ref, m1_all, ma_send, ma_recv, q, zz, rr, q).wait()
        m_copy(m2_ref, m2_all, mb_send, mb_recv, q, zz, rr, q).wait()
        return carry

    lax.fori_loop(1, N, wait_spread, 0)

    def wait_second(e, carry):
        src = lax.rem(z + e, Z)
        second(src, src).wait_recv()
        return carry

    lax.fori_loop(1, Z, wait_second, 0)

    def add_second(i, carry):
        part = pl.ds(pl.multiple_of(i * TILE, TILE), TILE)
        total = grad[part, :]
        for e in range(1, Z):
            total = total + recv2[lax.rem(z + e, Z), part, :].astype(jnp.float32)
        grad[part, :] = total
        return carry

    lax.fori_loop(0, DH // TILE, add_second, 0)

    projected = contract_rows(f_all[...], grad[...].astype(jnp.bfloat16))
    new_first = 0.8 * m1_all[...] + 0.2 * projected
    new_second = 0.9 * m2_all[...] + 0.1 * projected * projected
    nf_col[...] = new_first
    ns_col[...] = new_second
    dir_low = (new_first / (jnp.sqrt(new_second) + 1e-08)).astype(jnp.bfloat16)
    proj_low = projected.astype(jnp.bfloat16)
    dir_wide = dir_low.astype(jnp.float32)
    proj_wide = proj_low.astype(jnp.float32)
    stat[0] = jnp.broadcast_to(jnp.sum(dir_wide * dir_wide, axis=0, keepdims=True), (8, LANES))
    stat[1] = jnp.broadcast_to(jnp.sum(proj_wide * proj_wide, axis=0, keepdims=True), (8, LANES))
    stat_all[every] = stat[...]

    def s_copy(p, slot_of):
        q = lax.rem(every + p, N * T)
        d = q // T
        slot = slot_of(q)
        return pltpu.make_async_remote_copy(
            src_ref=stat, dst_ref=stat_all.at[slot],
            send_sem=st_send.at[q], recv_sem=st_recv.at[slot],
            device_id=device(d // R, lax.rem(d, R), lax.rem(q, T)), device_id_type=MESH,
        )

    def send_stat(p, carry):
        s_copy(p, lambda q: every).start()
        return carry

    lax.fori_loop(1, N * T, send_stat, 0)

    def back_copy(src, dst, size, ss, rs, q, zz, rr, sz, sr, slot):
        return pltpu.make_async_remote_copy(
            src_ref=src.at[rows(q, size), :], dst_ref=dst.at[:, column(sz, sr)],
            send_sem=ss.at[q], recv_sem=rs.at[slot],
            device_id=device(zz, rr, t), device_id_type=MESH,
        )

    def send_moments(p, carry):
        q, zz, rr = peer(p)
        back_copy(nf_col, nf_ref, MR, nf_send, nf_recv, q, zz, rr, z, r, me).start()
        back_copy(ns_col, ns_ref, MR, ns_send, ns_recv, q, zz, rr, z, r, me).start()
        return carry

    lax.fori_loop(1, N, send_moments, 0)
    nf_ref[:, column(z, r)] = nf_col[rows(me, MR), :]
    ns_ref[:, column(z, r)] = ns_col[rows(me, MR), :]

    upd_col[...] = jnp.dot(f_all[...], dir_low, preferred_element_type=jnp.float32)
    grad[...] = grad[...] - jnp.dot(f_all[...], proj_low, preferred_element_type=jnp.float32)

    def wait_stat(p, carry):
        s_copy(p, lambda q: q).wait()
        return carry

    lax.fori_loop(1, N * T, wait_stat, 0)
    totals = jnp.sum(stat_all[...], axis=0)
    dir_sum = jnp.sum(totals[0, 0:1, :], axis=1, keepdims=True)
    proj_sum = jnp.sum(totals[1, 0:1, :], axis=1, keepdims=True)
    scale_ratio = jnp.sqrt(dir_sum) / jnp.sqrt(proj_sum + 1e-06)
    upd_col[...] = upd_col[...] + scale_ratio * grad[...]

    def send_update(p, carry):
        q, zz, rr = peer(p)
        back_copy(upd_col, upd_ref, FR, up_send, up_recv, q, zz, rr, z, r, me).start()
        return carry

    lax.fori_loop(1, N, send_update, 0)
    upd_ref[:, column(z, r)] = upd_col[rows(me, FR), :]

    def wait_update(p, carry):
        q, zz, rr = peer(p)
        back_copy(upd_col, upd_ref, FR, up_send, up_recv, q, zz, rr, zz, rr, q).wait()
        return carry

    lax.fori_loop(1, N, wait_update, 0)

    new_weight = w_ref[...] - 0.01 * upd_ref[...]
    nw_ref[...] = new_weight
    wc_ref[rows(me, FR), :] = new_weight.astype(jnp.bfloat16)

    def along_z(zz, src):
        block = wc_ref.at[rows(src * R + r, FR), :]
        return pltpu.make_async_remote_copy(
            src_ref=block, dst_ref=block, send_sem=gz_send.at[zz], recv_sem=gz_recv.at[src],
            device_id=device(zz, r, t), device_id_type=MESH,
        )

    def along_r(rr, zz, src):
        block = wc_ref.at[rows(zz * R + src, FR), :]
        return pltpu.make_async_remote_copy(
            src_ref=block, dst_ref=block, send_sem=gr_send.at[rr, zz], recv_sem=gr_recv.at[src, zz],
            device_id=device(z, rr, t), device_id_type=MESH,
        )

    def start_z(e, carry):
        along_z(lax.rem(z + e, Z), z).start()
        return carry

    lax.fori_loop(1, Z, start_z, 0)

    def relay(e, carry):
        zz = lax.rem(z + Z - e, Z)

        @pl.when(e > 0)
        def _():
            along_z(zz, zz).wait_recv()

        def start_r(d, carry):
            along_r(lax.rem(r + d, R), zz, r).start()
            return carry

        return lax.fori_loop(1, R, start_r, carry)

    lax.fori_loop(0, Z, relay, 0)

    def drain(i, carry):
        zz = i // (R - 1)
        rr = lax.rem(r + 1 + lax.rem(i, R - 1), R)
        along_r(rr, zz, rr).wait()
        first(rr, zz, r).wait_send()
        return carry

    lax.fori_loop(0, Z * (R - 1), drain, 0)

    def drain_z(e, carry):
        zz = lax.rem(z + e, Z)
        along_z(zz, z).wait_send()
        second(zz, z).wait_send()
        return carry

    lax.fori_loop(1, Z, drain_z, 0)

    def drain_moments(p, carry):
        q, zz, rr = peer(p)
        back_copy(nf_col, nf_ref, MR, nf_send, nf_recv, q, zz, rr, zz, rr, q).wait()
        back_copy(ns_col, ns_ref, MR, ns_send, ns_recv, q, zz, rr, zz, rr, q).wait()
        return carry

    lax.fori_loop(1, N, drain_moments, 0)


def fused(Z, R, T, *args):
    mixer_out, out_grad, factors, weight, first_moment, second_moment = args
    N = Z * R
    DH = mixer_out.shape[1]
    rank = factors.shape[1]
    f32, bf16 = jnp.float32, jnp.bfloat16
    vmem = pl.BlockSpec(memory_space=pltpu.VMEM)
    dma = pltpu.SemaphoreType.DMA
    wide = lambda n: [dma((n,)), dma((n,))]
    return pl.pallas_call(
        functools.partial(fused_kernel, Z, R, T),
        out_shape=(
            jax.ShapeDtypeStruct(weight.shape, f32),
            jax.ShapeDtypeStruct(weight.shape, f32),
            jax.ShapeDtypeStruct(first_moment.shape, f32),
            jax.ShapeDtypeStruct(first_moment.shape, f32),
            jax.ShapeDtypeStruct((DH, weight.shape[1]), bf16),
        ),
        in_specs=[vmem] * 6,
        out_specs=(vmem,) * 5,
        scratch_shapes=[
            pltpu.VMEM((DH, mixer_out.shape[0]), bf16),
            pltpu.VMEM((R, Z, DH, LANES), bf16),
            pltpu.VMEM((R, Z, DH, LANES), bf16),
            pltpu.VMEM((Z, DH, LANES), f32),
            pltpu.VMEM((Z, DH, LANES), bf16),
            pltpu.VMEM((Z, DH, LANES), bf16),
            pltpu.VMEM((DH, LANES), f32),
            pltpu.VMEM((DH, rank), bf16),
            pltpu.VMEM((rank, LANES), f32),
            pltpu.VMEM((rank, LANES), f32),
            pltpu.VMEM((rank, LANES), f32),
            pltpu.VMEM((rank, LANES), f32),
            pltpu.VMEM((DH, LANES), f32),
            pltpu.VMEM((2, 8, LANES), f32),
            pltpu.VMEM((N * T, 2, 8, LANES), f32),
            dma((R, Z)), dma((R, Z)), *wide(Z),
            *wide(N), *wide(N), *wide(N),
            *wide(N * T), *wide(N), *wide(N), *wide(N),
            *wide(Z), dma((R, Z)), dma((R, Z)),
        ],
        compiler_params=pltpu.CompilerParams(
            collective_id=0, has_side_effects=True, vmem_limit_bytes=60 * 1024 * 1024
        ),
    )(*args)

def plain(mixer_out, out_grad, factors, weight, first_moment, second_moment):
    columns = mixer_out
    gradient = lax.psum_scatter(
        contract_rows(columns, out_grad), ("fs", "rep"), scatter_dimension=0, tiled=True
    )
    grad_low = gradient.astype(jnp.bfloat16)
    columns = factors
    projected = lax.psum_scatter(
        contract_rows(columns, grad_low), ("fs", "rep"), scatter_dimension=0, tiled=True
    )
    new_first = 0.8 * first_moment + 0.2 * projected
    new_second = 0.9 * second_moment + 0.1 * projected * projected
    direction = new_first / (jnp.sqrt(new_second) + 1e-08)
    dir_low = direction.astype(jnp.bfloat16)
    proj_low = projected.astype(jnp.bfloat16)
    dir_whole, proj_whole = (
        lax.all_gather(dir_low, ("fs", "rep"), axis=0, tiled=True),
        lax.all_gather(proj_low, ("fs", "rep"), axis=0, tiled=True),
    )
    dir_wide = dir_low.astype(jnp.float32)
    proj_wide = proj_low.astype(jnp.float32)
    dir_sum, proj_sum = lax.psum(
        (jnp.sum(dir_wide * dir_wide), jnp.sum(proj_wide * proj_wide)), ("fs", "rep", "tp")
    )
    back_dir = jnp.dot(factors, dir_whole, preferred_element_type=jnp.float32)
    back_proj = jnp.dot(factors, proj_whole, preferred_element_type=jnp.float32)
    scale_ratio = jnp.sqrt(dir_sum) / jnp.sqrt(proj_sum + 1e-06)
    update = back_dir + scale_ratio * (gradient - back_proj)
    new_weight = weight - 0.01 * update
    weight_copy = lax.all_gather(new_weight.astype(jnp.bfloat16), ("fs", "rep"), axis=0, tiled=True)
    return (new_weight, update, new_first, new_second, weight_copy)


def solution(mesh):
    Z, R, T = mesh.shape["fs"], mesh.shape["rep"], mesh.shape["tp"]

    def per_device(*args):
        mixer_out, out_grad, factors, weight, first_moment, second_moment = args
        fits = (
            out_grad.shape[1] == Z * R * LANES
            and mixer_out.shape[1] % TILE == 0
            and weight.shape[0] % 16 == 0
            and first_moment.shape[0] % 8 == 0
            and min(Z, R) > 1
        )
        return fused(Z, R, T, *args) if fits else plain(*args)

    in_specs = (
        P(("fs", "rep"), None),
        P(("fs", "rep"), "tp"),
        P(("fs", "rep"), None),
        P(("fs", "rep"), "tp"),
        P(("fs", "rep"), "tp"),
        P(("fs", "rep"), "tp"),
    )
    out_specs = (
        P(("fs", "rep"), "tp"),
        P(("fs", "rep"), "tp"),
        P(("fs", "rep"), "tp"),
        P(("fs", "rep"), "tp"),
        P(None, "tp"),
    )
    return jax.shard_map(
        per_device, mesh=mesh, in_specs=in_specs, out_specs=out_specs, check_vma=False
    )
```

```python
import functools

import jax
import jax.numpy as jnp
from jax import lax
from jax.experimental import pallas as pl
from jax.experimental.pallas import tpu as pltpu
from jax.sharding import PartitionSpec as P

MESH = pl.DeviceIdType.MESH
LANES = 128
TILE = 256


def contract_rows(left, right):
    return lax.dot_general(
        left, right, (((0,), (0,)), ((), ())), preferred_element_type=jnp.float32
    )


def fused_kernel(
    Z, R, T,
    m_ref, o_ref, f_ref, w_ref, m1_ref, m2_ref,
    nw_ref, upd_ref, nf_ref, ns_ref, wc_ref,
    mt, send1, recv1, own, send2, recv2, grad, f_all, m1_all, m2_all,
    nf_col, ns_col, upd_col, stat, stat_all,
    s1_send, s1_recv, s2_send, s2_recv,
    fa_send, fa_recv, ma_send, ma_recv, mb_send, mb_recv,
    st_send, st_recv, nf_send, nf_recv, ns_send, ns_recv, up_send, up_recv,
    gz_send, gz_recv, gr_send, gr_recv,
    recvd, d_send, d_recv, gh_send, gh_recv,
):
    N = Z * R
    z, r, t = lax.axis_index("fs"), lax.axis_index("rep"), lax.axis_index("tp")
    me = z * R + r
    every = me * T + t
    DH = m_ref.shape[1]
    FR = f_ref.shape[0]
    MR = m1_ref.shape[0]
    H, TH, FH = DH // 2, DH // TILE // 2, FR // 2
    xn, yn, dn = r + 1 - 2 * lax.rem(r, 2), lax.rem(r + 2, R), R - 1 - r

    def device(zz, rr, tt):
        return {"fs": zz, "rep": rr, "tp": tt}

    def peer(p):
        q = lax.rem(me + p, N)
        return q, q // R, lax.rem(q, R)

    def column(zz, rr):
        return pl.ds(pl.multiple_of((rr * Z + zz) * LANES, LANES), LANES)

    def rows(q, size):
        return pl.ds(pl.multiple_of(q * size, size), size)

    barrier = pltpu.get_barrier_semaphore()

    def greet(p, carry):
        q = lax.rem(every + p, N * T)
        d = q // T
        pl.semaphore_signal(
            barrier, inc=1, device_id=device(d // R, lax.rem(d, R), lax.rem(q, T)), device_id_type=MESH
        )
        return carry

    lax.fori_loop(1, N * T, greet, 0)

    def turn(i, carry):
        part = pl.ds(pl.multiple_of(i * TILE, TILE), TILE)
        mt[part, :] = m_ref[:, part].T
        return carry

    lax.fori_loop(0, DH // TILE, turn, 0)
    pl.semaphore_wait(barrier, N * T - 1)

    def product(zz, rr, store, lo=0, hi=None):
        cols = column(zz, rr)

        def tile(i, carry):
            part = pl.ds(pl.multiple_of(i * TILE, TILE), TILE)
            store(part, jnp.dot(mt[part, :], o_ref[:, cols], preferred_element_type=jnp.float32))
            return carry

        lax.fori_loop(lo, DH // TILE if hi is None else hi, tile, 0)

    def first(rr, zz, src):
        return pltpu.make_async_remote_copy(
            src_ref=send1.at[rr, zz], dst_ref=recv1.at[src, zz],
            send_sem=s1_send.at[rr, zz], recv_sem=s1_recv.at[src, zz],
            device_id=device(z, rr, t), device_id_type=MESH,
        )

    def second(zz, src):
        return pltpu.make_async_remote_copy(
            src_ref=send2.at[zz], dst_ref=recv2.at[src],
            send_sem=s2_send.at[zz], recv_sem=s2_recv.at[src],
            device_id=device(zz, r, t), device_id_type=MESH,
        )

    def via(h, zz):
        return pltpu.make_async_remote_copy(
            src_ref=send1.at[dn, zz, pl.ds(h * H, H), :], dst_ref=recvd.at[h, zz],
            send_sem=d_send.at[h, zz], recv_sem=d_recv.at[h, zz],
            device_id=device(z, yn if h else xn, t), device_id_type=MESH,
        )

    def across(e, carry):
        zz = lax.rem(z + 1 + e, Z)

        def store(part, value):
            send1[dn, zz, part, :] = value.astype(jnp.bfloat16)

        product(zz, dn, store)
        via(0, zz).start()
        via(1, zz).start()
        return carry

    lax.fori_loop(0, Z, across, 0)

    def beside(e, carry):
        zz = lax.rem(z + 1 + e, Z)
        for h, rr in ((1, xn), (0, yn)):

            def store(part, value):
                send1[rr, zz, part, :] = value.astype(jnp.bfloat16)

            def store_sum(part, value):
                inner = pl.ds(pl.multiple_of(part.start - h * H, TILE), TILE)
                total = value + recvd[h, zz, inner, :].astype(jnp.float32)
                send1[rr, zz, part, :] = total.astype(jnp.bfloat16)

            product(zz, rr, store, (1 - h) * TH, (2 - h) * TH)
            via(h, zz).wait_recv()
            product(zz, rr, store_sum, h * TH, (h + 1) * TH)
            first(rr, zz, r).start()
        return carry

    lax.fori_loop(0, Z, beside, 0)

    def f_copy(q, zz, rr, slot):
        return pltpu.make_async_remote_copy(
            src_ref=f_ref, dst_ref=f_all.at[rows(slot, FR), :],
            send_sem=fa_send.at[q], recv_sem=fa_recv.at[slot],
            device_id=device(zz, rr, t), device_id_type=MESH,
        )

    def m_copy(src, dst, ss, rs, q, zz, rr, slot):
        return pltpu.make_async_remote_copy(
            src_ref=src.at[:, column(zz, rr)], dst_ref=dst.at[rows(slot, MR), :],
            send_sem=ss.at[q], recv_sem=rs.at[slot],
            device_id=device(zz, rr, t), device_id_type=MESH,
        )

    def spread(p, carry):
        q, zz, rr = peer(p)
        f_copy(q, zz, rr, me).start()
        m_copy(m1_ref, m1_all, ma_send, ma_recv, q, zz, rr, me).start()
        m_copy(m2_ref, m2_all, mb_send, mb_recv, q, zz, rr, me).start()
        return carry

    lax.fori_loop(1, N, spread, 0)
    f_all[rows(me, FR), :] = f_ref[...]
    m1_all[rows(me, MR), :] = m1_ref[:, column(z, r)]
    m2_all[rows(me, MR), :] = m2_ref[:, column(z, r)]

    def own_block(i, carry):
        def store(part, value):
            own[i, part, :] = value

        product(i, r, store)
        return carry

    lax.fori_loop(0, Z, own_block, 0)

    def join(zz, store):
        for src in (xn, yn):
            first(src, zz, src).wait_recv()

        def tile(i, carry):
            part = pl.ds(pl.multiple_of(i * TILE, TILE), TILE)
            total = own[zz, part, :]
            for src in (xn, yn):
                total = total + recv1[src, zz, part, :].astype(jnp.float32)
            store(part, total)
            return carry

        lax.fori_loop(0, DH // TILE, tile, 0)

    def phase2(e, carry):
        zz = lax.rem(z + e, Z)

        def store(part, value):
            send2[zz, part, :] = value.astype(jnp.bfloat16)

        join(zz, store)
        second(zz, z).start()
        return carry

    lax.fori_loop(1, Z, phase2, 0)

    def store_own(part, value):
        grad[part, :] = value

    join(z, store_own)

    def wait_spread(p, carry):
        q, zz, rr = peer(p)
        f_copy(q, zz, rr, q).wait()
        m_copy(m1_ref, m1_all, ma_send, ma_recv, q, zz, rr, q).wait()
        m_copy(m2_ref, m2_all, mb_send, mb_recv, q, zz, rr, q).wait()
        return carry

    lax.fori_loop(1, N, wait_spread, 0)

    def wait_second(e, carry):
        src = lax.rem(z + e, Z)
        second(src, src).wait_recv()
        return carry

    lax.fori_loop(1, Z, wait_second, 0)

    def add_second(i, carry):
        part = pl.ds(pl.multiple_of(i * TILE, TILE), TILE)
        total = grad[part, :]
        for e in range(1, Z):
            total = total + recv2[lax.rem(z + e, Z), part, :].astype(jnp.float32)
        grad[part, :] = total
        return carry

    lax.fori_loop(0, DH // TILE, add_second, 0)

    projected = contract_rows(f_all[...], grad[...].astype(jnp.bfloat16))
    new_first = 0.8 * m1_all[...] + 0.2 * projected
    new_second = 0.9 * m2_all[...] + 0.1 * projected * projected
    nf_col[...] = new_first
    ns_col[...] = new_second
    dir_low = (new_first / (jnp.sqrt(new_second) + 1e-08)).astype(jnp.bfloat16)
    proj_low = projected.astype(jnp.bfloat16)
    dir_wide = dir_low.astype(jnp.float32)
    proj_wide = proj_low.astype(jnp.float32)
    stat[0] = jnp.broadcast_to(jnp.sum(dir_wide * dir_wide, axis=0, keepdims=True), (8, LANES))
    stat[1] = jnp.broadcast_to(jnp.sum(proj_wide * proj_wide, axis=0, keepdims=True), (8, LANES))
    stat_all[every] = stat[...]

    def s_copy(p, slot_of):
        q = lax.rem(every + p, N * T)
        d = q // T
        slot = slot_of(q)
        return pltpu.make_async_remote_copy(
            src_ref=stat, dst_ref=stat_all.at[slot],
            send_sem=st_send.at[q], recv_sem=st_recv.at[slot],
            device_id=device(d // R, lax.rem(d, R), lax.rem(q, T)), device_id_type=MESH,
        )

    def send_stat(p, carry):
        s_copy(p, lambda q: every).start()
        return carry

    lax.fori_loop(1, N * T, send_stat, 0)

    def back_copy(src, dst, size, ss, rs, q, zz, rr, sz, sr, slot):
        return pltpu.make_async_remote_copy(
            src_ref=src.at[rows(q, size), :], dst_ref=dst.at[:, column(sz, sr)],
            send_sem=ss.at[q], recv_sem=rs.at[slot],
            device_id=device(zz, rr, t), device_id_type=MESH,
        )

    def send_moments(p, carry):
        q, zz, rr = peer(p)
        back_copy(nf_col, nf_ref, MR, nf_send, nf_recv, q, zz, rr, z, r, me).start()
        back_copy(ns_col, ns_ref, MR, ns_send, ns_recv, q, zz, rr, z, r, me).start()
        return carry

    lax.fori_loop(1, N, send_moments, 0)
    nf_ref[:, column(z, r)] = nf_col[rows(me, MR), :]
    ns_ref[:, column(z, r)] = ns_col[rows(me, MR), :]

    upd_col[...] = jnp.dot(f_all[...], dir_low, preferred_element_type=jnp.float32)
    grad[...] = grad[...] - jnp.dot(f_all[...], proj_low, preferred_element_type=jnp.float32)

    def wait_stat(p, carry):
        s_copy(p, lambda q: q).wait()
        return carry

    lax.fori_loop(1, N * T, wait_stat, 0)
    totals = jnp.sum(stat_all[...], axis=0)
    dir_sum = jnp.sum(totals[0, 0:1, :], axis=1, keepdims=True)
    proj_sum = jnp.sum(totals[1, 0:1, :], axis=1, keepdims=True)
    scale_ratio = jnp.sqrt(dir_sum) / jnp.sqrt(proj_sum + 1e-06)
    upd_col[...] = upd_col[...] + scale_ratio * grad[...]

    def send_update(p, carry):
        q, zz, rr = peer(p)
        back_copy(upd_col, upd_ref, FR, up_send, up_recv, q, zz, rr, z, r, me).start()
        return carry

    lax.fori_loop(1, N, send_update, 0)
    upd_ref[:, column(z, r)] = upd_col[rows(me, FR), :]

    def wait_update(p, carry):
        q, zz, rr = peer(p)
        back_copy(upd_col, upd_ref, FR, up_send, up_recv, q, zz, rr, zz, rr, q).wait()
        return carry

    lax.fori_loop(1, N, wait_update, 0)

    new_weight = w_ref[...] - 0.01 * upd_ref[...]
    nw_ref[...] = new_weight
    wc_ref[rows(me, FR), :] = new_weight.astype(jnp.bfloat16)

    def along_z(zz, src):
        block = wc_ref.at[rows(src * R + r, FR), :]
        return pltpu.make_async_remote_copy(
            src_ref=block, dst_ref=block, send_sem=gz_send.at[zz], recv_sem=gz_recv.at[src],
            device_id=device(zz, r, t), device_id_type=MESH,
        )

    def along_r(rr, zz, src):
        block = wc_ref.at[rows(zz * R + src, FR), :]
        return pltpu.make_async_remote_copy(
            src_ref=block, dst_ref=block, send_sem=gr_send.at[rr, zz], recv_sem=gr_recv.at[src, zz],
            device_id=device(z, rr, t), device_id_type=MESH,
        )

    def start_z(e, carry):
        along_z(lax.rem(z + e, Z), z).start()
        return carry

    lax.fori_loop(1, Z, start_z, 0)

    def half(h, zz, src):
        block = wc_ref.at[pl.ds(pl.multiple_of((zz * R + src) * FR + h * FH, FH), FH), :]
        return pltpu.make_async_remote_copy(
            src_ref=block, dst_ref=block, send_sem=gh_send.at[h, zz], recv_sem=gh_recv.at[h, zz],
            device_id=device(z, xn if h else yn, t), device_id_type=MESH,
        )

    def relay(e, carry):
        zz = lax.rem(z + 2 * Z - e, Z)
        last = lax.rem(z + 2 * Z - e + 1, Z)

        @pl.when(e < Z)
        def _():
            @pl.when(e > 0)
            def _():
                along_z(zz, zz).wait_recv()

            along_r(xn, zz, r).start()
            along_r(yn, zz, r).start()

        @pl.when(e > 0)
        def _():
            along_r(xn, last, xn).wait_recv()
            half(0, last, xn).start()
            along_r(yn, last, yn).wait_recv()
            half(1, last, yn).start()

        return carry

    lax.fori_loop(0, Z + 1, relay, 0)

    def drain(zz, carry):
        for h, rr in ((0, xn), (1, yn)):
            along_r(rr, zz, r).wait_send()
            first(rr, zz, r).wait_send()
            via(h, zz).wait_send()
            half(h, zz, rr).wait_send()
            half(h, zz, dn).wait_recv()
        return carry

    lax.fori_loop(0, Z, drain, 0)

    def drain_z(e, carry):
        zz = lax.rem(z + e, Z)
        along_z(zz, z).wait_send()
        second(zz, z).wait_send()
        return carry

    lax.fori_loop(1, Z, drain_z, 0)

    def drain_moments(p, carry):
        q, zz, rr = peer(p)
        back_copy(nf_col, nf_ref, MR, nf_send, nf_recv, q, zz, rr, zz, rr, q).wait()
        back_copy(ns_col, ns_ref, MR, ns_send, ns_recv, q, zz, rr, zz, rr, q).wait()
        return carry

    lax.fori_loop(1, N, drain_moments, 0)


def fused(Z, R, T, *args):
    mixer_out, out_grad, factors, weight, first_moment, second_moment = args
    N = Z * R
    DH = mixer_out.shape[1]
    rank = factors.shape[1]
    f32, bf16 = jnp.float32, jnp.bfloat16
    vmem = pl.BlockSpec(memory_space=pltpu.VMEM)
    dma = pltpu.SemaphoreType.DMA
    wide = lambda n: [dma((n,)), dma((n,))]
    return pl.pallas_call(
        functools.partial(fused_kernel, Z, R, T),
        out_shape=(
            jax.ShapeDtypeStruct(weight.shape, f32),
            jax.ShapeDtypeStruct(weight.shape, f32),
            jax.ShapeDtypeStruct(first_moment.shape, f32),
            jax.ShapeDtypeStruct(first_moment.shape, f32),
            jax.ShapeDtypeStruct((DH, weight.shape[1]), bf16),
        ),
        in_specs=[vmem] * 6,
        out_specs=(vmem,) * 5,
        scratch_shapes=[
            pltpu.VMEM((DH, mixer_out.shape[0]), bf16),
            pltpu.VMEM((R, Z, DH, LANES), bf16),
            pltpu.VMEM((R, Z, DH, LANES), bf16),
            pltpu.VMEM((Z, DH, LANES), f32),
            pltpu.VMEM((Z, DH, LANES), bf16),
            pltpu.VMEM((Z, DH, LANES), bf16),
            pltpu.VMEM((DH, LANES), f32),
            pltpu.VMEM((DH, rank), bf16),
            pltpu.VMEM((rank, LANES), f32),
            pltpu.VMEM((rank, LANES), f32),
            pltpu.VMEM((rank, LANES), f32),
            pltpu.VMEM((rank, LANES), f32),
            pltpu.VMEM((DH, LANES), f32),
            pltpu.VMEM((2, 8, LANES), f32),
            pltpu.VMEM((N * T, 2, 8, LANES), f32),
            dma((R, Z)), dma((R, Z)), *wide(Z),
            *wide(N), *wide(N), *wide(N),
            *wide(N * T), *wide(N), *wide(N), *wide(N),
            *wide(Z), dma((R, Z)), dma((R, Z)),
            pltpu.VMEM((2, Z, DH // 2, LANES), bf16),
            dma((2, Z)), dma((2, Z)), dma((2, Z)), dma((2, Z)),
        ],
        compiler_params=pltpu.CompilerParams(
            collective_id=0, has_side_effects=True, vmem_limit_bytes=60 * 1024 * 1024
        ),
    )(*args)

def plain(mixer_out, out_grad, factors, weight, first_moment, second_moment):
    columns = mixer_out
    gradient = lax.psum_scatter(
        contract_rows(columns, out_grad), ("fs", "rep"), scatter_dimension=0, tiled=True
    )
    grad_low = gradient.astype(jnp.bfloat16)
    columns = factors
    projected = lax.psum_scatter(
        contract_rows(columns, grad_low), ("fs", "rep"), scatter_dimension=0, tiled=True
    )
    new_first = 0.8 * first_moment + 0.2 * projected
    new_second = 0.9 * second_moment + 0.1 * projected * projected
    direction = new_first / (jnp.sqrt(new_second) + 1e-08)
    dir_low = direction.astype(jnp.bfloat16)
    proj_low = projected.astype(jnp.bfloat16)
    dir_whole, proj_whole = (
        lax.all_gather(dir_low, ("fs", "rep"), axis=0, tiled=True),
        lax.all_gather(proj_low, ("fs", "rep"), axis=0, tiled=True),
    )
    dir_wide = dir_low.astype(jnp.float32)
    proj_wide = proj_low.astype(jnp.float32)
    dir_sum, proj_sum = lax.psum(
        (jnp.sum(dir_wide * dir_wide), jnp.sum(proj_wide * proj_wide)), ("fs", "rep", "tp")
    )
    back_dir = jnp.dot(factors, dir_whole, preferred_element_type=jnp.float32)
    back_proj = jnp.dot(factors, proj_whole, preferred_element_type=jnp.float32)
    scale_ratio = jnp.sqrt(dir_sum) / jnp.sqrt(proj_sum + 1e-06)
    update = back_dir + scale_ratio * (gradient - back_proj)
    new_weight = weight - 0.01 * update
    weight_copy = lax.all_gather(new_weight.astype(jnp.bfloat16), ("fs", "rep"), axis=0, tiled=True)
    return (new_weight, update, new_first, new_second, weight_copy)


def solution(mesh):
    Z, R, T = mesh.shape["fs"], mesh.shape["rep"], mesh.shape["tp"]

    def per_device(*args):
        mixer_out, out_grad, factors, weight, first_moment, second_moment = args
        fits = (
            out_grad.shape[1] == Z * R * LANES
            and mixer_out.shape[1] % (2 * TILE) == 0
            and weight.shape[0] % 32 == 0
            and first_moment.shape[0] % 8 == 0
            and R == 4
            and Z > 1
        )
        return fused(Z, R, T, *args) if fits else plain(*args)

    in_specs = (
        P(("fs", "rep"), None),
        P(("fs", "rep"), "tp"),
        P(("fs", "rep"), None),
        P(("fs", "rep"), "tp"),
        P(("fs", "rep"), "tp"),
        P(("fs", "rep"), "tp"),
    )
    out_specs = (
        P(("fs", "rep"), "tp"),
        P(("fs", "rep"), "tp"),
        P(("fs", "rep"), "tp"),
        P(("fs", "rep"), "tp"),
        P(None, "tp"),
    )
    return jax.shard_map(
        per_device, mesh=mesh, in_specs=in_specs, out_specs=out_specs, check_vma=False
    )
```
